32 devices in a mesh: grp: 2 (over y), fs: 4 (over z), tp: 4 (over x, core).
Axes of the slice: x: 2, y: 2, z: 4, core: 2. Of those that a mesh axis runs over, the one named last changes fastest.
Arguments:
- tokens: bfloat16 [8192, 2048], P(('grp', 'fs', 'tp')), parts along dimension 0, may hold values from -6 to 6
- first_gain: float32 [2048], replicated, may hold values from 0.1 to 1.9
- mixer_gain: float32 [2048], replicated, may hold values from 0.1 to 1.9
- gate_weight: bfloat16 [2048, 4608], P('fs', 'tp'), may hold values from -0.125 to 0.125
- up_weight: bfloat16 [2048, 4608], P('fs', 'tp'), may hold values from -0.125 to 0.125
- down_weight: bfloat16 [4608, 2048], P('tp', 'fs'), may hold values from -0.09375 to 0.09375
- query_weight: bfloat16 [2048, 2048], P('fs', 'tp'), may hold values from -0.125 to 0.125
- key_weight: bfloat16 [2048, 2048], P('fs', 'tp'), may hold values from -0.125 to 0.125
- value_weight: bfloat16 [2048, 4096], P('fs', 'tp'), may hold values from -0.125 to 0.125
- head_gain: float32 [4096], P('tp'), may hold values from 0.1 to 1.9
- out_weight: bfloat16 [4096, 2048], P('tp', 'fs'), may hold values from -0.09375 to 0.09375
- log_decay: float32 [2, 8], P(None, 'tp'), may hold values from -0.03125 to 0, as said below
Outputs:
- updated: bfloat16 [8192, 2048], P(('grp', 'fs', 'tp')), parts along dimension 0
The draws below stay inside these ranges and needn't reach their ends.
There are 2 independent parts, one for each index of `grp`. The reference program is written for one: setup_inputs(seed, part) draws one part's arguments, and reference() takes and returns one part's arrays. A program takes and returns all parts, laid end to end along the dimension named above; an argument that names none is the same for every part. Nothing has to cross between parts.
Inputs may be any that keep to these rules, and one draw needn't show every extreme that they name: `log_decay`: log decay per step of each direction (forward, then backward) and head.
All inputs are finite; a program needn't handle non-finite values.
Results may differ from the reference program's by a relative error of at most 0.02.
Values may be sent and summed in bfloat16 or wider, within the bound.
A program may use at most 64 MiB of HBM per device.

```python
import math
import jax
import jax.numpy as jnp
from jax import lax

D = 2048
H = 8
DK = 256
DV = 512
FF = 4608
BLOCK = 128
TOK = 1024
TOKENS = 4096
N_TP = 4


def draw_log_decay(key, part):
    order = jax.random.permutation(jax.random.fold_in(key, 11), H)
    fast_count = H // 2
    fast_heads = order < fast_count
    unit = jax.random.uniform(jax.random.fold_in(key, 12), (2, H), jnp.float32)
    slow_rate = math.log(0.1) / TOK * (0.1 + 0.9 * unit)
    fast_rate = -4.0 / BLOCK + unit * (4.0 / BLOCK - 4.0 / (3.0 * BLOCK))
    return jnp.where(fast_heads[None, :], fast_rate, slow_rate).astype(jnp.float32)


def block_scale(stream_key, shape, cuts, smallest, top_value):
    level, own = 1.0, jax.random.fold_in(stream_key, 6)
    for position, parts in cuts:
        heights = jnp.exp(jax.random.uniform(jax.random.fold_in(own, position), (parts,), jnp.float32, smallest / len(cuts), top_value / len(cuts)))
        level = level * jnp.repeat(heights, shape[position] // parts).reshape([-1 if axis == position else 1 for axis in range(len(shape))])
    return level


def centred(own_key, dims, scale, limit, cuts=(), held_as=jnp.bfloat16):
    level = block_scale(own_key, dims, cuts, -0.22, 0.18) if cuts else 1.0
    drawn = jax.random.normal(own_key, dims, jnp.float32) * scale * level
    return jnp.minimum(jnp.maximum(drawn, -limit), limit).astype(held_as)


def setup_inputs(seed: int = 0, part: int = 0) -> dict:
    arg_keys = jax.random.split(jax.random.key(seed), 13)
    part_splits = jax.random.split(jax.random.fold_in(arg_keys[12], part), 13)
    tokens = centred(part_splits[0], (TOKENS, D), 1.0, 6.0, ((0, 16),))
    first_gain = jnp.clip(1.0 + 0.18 * jax.random.normal(arg_keys[1], (D,), jnp.float32), 0.1, 1.9)
    mixer_gain = jnp.clip(1.0 + 0.18 * jax.random.normal(arg_keys[2], (D,), jnp.float32), 0.1, 1.9)
    gate_weight = centred(arg_keys[3], (D, FF), D ** -0.5, 0.125, ((0, 4), (1, 4)))
    up_weight = centred(arg_keys[4], (D, FF), D ** -0.5, 0.125, ((0, 4), (1, 4)))
    down_weight = centred(arg_keys[5], (FF, D), FF ** -0.5, 0.09375, ((0, 4), (1, 4)))
    query_weight = centred(arg_keys[6], (D, H * DK), D ** -0.5, 0.125, ((0, 4), (1, 4)))
    key_weight = centred(arg_keys[7], (D, H * DK), D ** -0.5, 0.125, ((0, 4), (1, 4)))
    value_weight = centred(arg_keys[8], (D, H * DV), D ** -0.5, 0.125, ((0, 4), (1, 4)))
    head_gain = jnp.clip(1.0 + 0.18 * jax.random.normal(arg_keys[9], (H * DV,), jnp.float32), 0.1, 1.9)
    out_weight = centred(arg_keys[10], (H * DV, D), (H * DV) ** -0.5, 0.09375, ((0, 4), (1, 4)))
    log_decay = draw_log_decay(jax.random.fold_in(arg_keys[12], 71), part)
    return {"tokens": tokens, "first_gain": first_gain, "mixer_gain": mixer_gain, "gate_weight": gate_weight, "up_weight": up_weight, "down_weight": down_weight, "query_weight": query_weight, "key_weight": key_weight, "value_weight": value_weight, "head_gain": head_gain, "out_weight": out_weight, "log_decay": log_decay}


EPS = 1e-06

def norm_rows(values, gain):
    widened = values.astype(jnp.float32)
    factor = lax.rsqrt(lax.optimization_barrier(jnp.mean(widened * widened, axis=-1, keepdims=True)) + EPS)
    return (widened * factor * gain).astype(jnp.bfloat16)

def split_sum(left, right, pieces):
    width = left.shape[1] // pieces
    running = jnp.zeros((left.shape[0], right.shape[1]), jnp.float32)
    for which_block in range(pieces):
        product = jnp.dot(left[:, which_block * width:(which_block + 1) * width], right[which_block * width:(which_block + 1) * width], preferred_element_type=jnp.float32)
        running = running + lax.optimization_barrier(product.astype(jnp.bfloat16)).astype(jnp.float32)
    return running

def sweep_one(queries, key_rows, value_rows, log_rate):
    length = queries.shape[0]
    block_count = length // BLOCK
    places = jnp.arange(BLOCK, dtype=jnp.float32)
    distance = places[:, None] - places[None, :]
    inner_decay = jnp.where(distance >= 0, jnp.exp(log_rate * jnp.maximum(distance, 0.0)), 0.0)
    enter_decay = jnp.exp(log_rate * (places + 1.0))
    leave_decay = jnp.exp(log_rate * (BLOCK - 1.0 - places))
    block_decay = jnp.exp(log_rate * BLOCK)
    highest = lax.Precision.HIGHEST

    def advance(memory, blocks):
        query_block, key_block, value_block = blocks
        scores = jnp.dot(query_block.astype(jnp.bfloat16), key_block.astype(jnp.bfloat16).T, preferred_element_type=jnp.float32) * inner_decay
        result = jnp.dot(scores, value_block, precision=highest)
        result = result + jnp.dot(query_block, memory, precision=highest) * enter_decay[:, None]
        memory = memory * block_decay + jnp.dot((key_block * leave_decay[:, None]).T, value_block, precision=highest)
        return (memory, result)
    start_memory = jnp.zeros((queries.shape[1], value_rows.shape[1]), jnp.float32)
    _, results = lax.scan(advance, start_memory, (queries.reshape(block_count, BLOCK, -1), key_rows.reshape(block_count, BLOCK, -1), value_rows.reshape(block_count, BLOCK, -1)))
    return results.reshape(length, -1)

def retain_both(queries, key_rows, value_rows, forward_rate, backward_rate):
    forward_part = sweep_one(queries, key_rows, value_rows, forward_rate)
    backward_part = sweep_one(jnp.flip(queries, axis=0), jnp.flip(key_rows, axis=0), jnp.flip(value_rows, axis=0), backward_rate)
    return forward_part + jnp.flip(backward_part, axis=0)

def head_norm(outputs, gain):
    heads_here = gain.shape[0] // DV
    centered = outputs - lax.optimization_barrier(jnp.mean(outputs, axis=-1, keepdims=True))
    variance = lax.optimization_barrier(jnp.mean(centered * centered, axis=-1, keepdims=True))
    return centered * lax.rsqrt(variance + EPS) * gain.reshape(heads_here, 1, DV)

def feed_half(residual, gain, gate_weight, up_weight, down_weight):
    normed = norm_rows(residual, gain)
    gate_sum = jnp.dot(normed, gate_weight, preferred_element_type=jnp.float32)
    up_sum = jnp.dot(normed, up_weight, preferred_element_type=jnp.float32)
    hidden = (jax.nn.silu(gate_sum) * up_sum).astype(jnp.bfloat16)
    branch = split_sum(hidden, down_weight, N_TP)
    return (residual.astype(jnp.float32) + 0.5 * branch).astype(jnp.bfloat16)

def to_heads(values, width):
    widened = lax.optimization_barrier(values.astype(jnp.bfloat16)).astype(jnp.float32)
    return widened.reshape(-1, TOK, H, width).transpose(0, 2, 1, 3)

def mix_tokens(residual, gain, query_weight, key_weight, value_weight, head_gain, out_weight, log_decay):
    normed = norm_rows(residual, gain)
    queries = to_heads(jnp.dot(normed, query_weight, preferred_element_type=jnp.float32), DK) * DK ** (-0.5)
    key_rows = to_heads(jnp.dot(normed, key_weight, preferred_element_type=jnp.float32), DK)
    value_rows = to_heads(jnp.dot(normed, value_weight, preferred_element_type=jnp.float32), DV)

    def per_sequence(blocks):
        return jax.vmap(retain_both)(blocks[0], blocks[1], blocks[2], log_decay[0], log_decay[1])
    outputs = lax.map(per_sequence, (queries, key_rows, value_rows))
    normed_heads = head_norm(outputs, head_gain).astype(jnp.bfloat16)
    flat = normed_heads.transpose(0, 2, 1, 3).reshape(-1, H * DV)
    branch = split_sum(flat, out_weight, N_TP)
    return (residual.astype(jnp.float32) + branch).astype(jnp.bfloat16)

def reference(tokens, first_gain, mixer_gain, gate_weight, up_weight, down_weight, query_weight, key_weight, value_weight, head_gain, out_weight, log_decay):
    after_first = feed_half(tokens, first_gain, gate_weight, up_weight, down_weight)
    return mix_tokens(after_first, mixer_gain, query_weight, key_weight, value_weight, head_gain, out_weight, log_decay)
```

```python
import functools

import jax
import jax.numpy as jnp
from jax import lax
from jax.experimental import pallas as pl
from jax.experimental.pallas import tpu as pltpu
from jax.sharding import PartitionSpec as P

DK = 256
DV = 512
EPS = 1e-06
LANES = 128


def norm_rows(values, gain):
    widened = values.astype(jnp.float32)
    factor = lax.rsqrt(jnp.mean(widened * widened, axis=-1, keepdims=True) + EPS)
    return (widened * factor * gain).astype(jnp.bfloat16)


def tile_of(width, top):
    best = width
    for tile in range(LANES, top + 1, LANES):
        if width % tile == 0:
            best = tile
    return best


def cost(flops, *arrays):
    return pl.CostEstimate(
        flops=flops,
        transcendentals=0,
        bytes_accessed=sum(a.size * a.dtype.itemsize for a in arrays),
    )


def gated_kernel(count, rows_ref, *refs):
    rows = rows_ref[...]
    gate = jnp.concatenate([r[...] for r in refs[:count]], axis=0)
    up = jnp.concatenate([r[...] for r in refs[count : 2 * count]], axis=0)
    gate_sum = jnp.dot(rows, gate, preferred_element_type=jnp.float32)
    up_sum = jnp.dot(rows, up, preferred_element_type=jnp.float32)
    refs[-1][...] = (gate_sum / (1.0 + jnp.exp(-gate_sum)) * up_sum).astype(jnp.bfloat16)


def gated(rows, gates, ups):
    count, depth, width = len(gates), rows.shape[1], gates[0].shape[1]
    tall, wide = tile_of(rows.shape[0], 512), tile_of(width, 384)
    piece = pl.BlockSpec((gates[0].shape[0], wide), lambda j, i: (0, j))
    return pl.pallas_call(
        functools.partial(gated_kernel, count),
        grid=(width // wide, rows.shape[0] // tall),
        in_specs=[pl.BlockSpec((tall, depth), lambda j, i: (i, 0))] + [piece] * (2 * count),
        out_specs=pl.BlockSpec((tall, wide), lambda j, i: (i, j)),
        out_shape=jax.ShapeDtypeStruct((rows.shape[0], width), jnp.bfloat16),
        cost_estimate=cost(4 * rows.size * width, rows, *gates, *ups),
    )(rows, *gates, *ups)


def deep_kernel(rows_ref, *refs):
    weight = jnp.concatenate([r[...] for r in refs[:-1]], axis=0)
    refs[-1][...] = jnp.dot(
        rows_ref[...], weight, preferred_element_type=jnp.float32
    ).astype(jnp.bfloat16)


def deep(rows, pieces):
    depth, width = rows.shape[1], pieces[0].shape[1]
    tall, wide = tile_of(rows.shape[0], 512), tile_of(width, 512)
    piece = pl.BlockSpec((pieces[0].shape[0], wide), lambda j, i: (0, j))
    return pl.pallas_call(
        deep_kernel,
        grid=(width // wide, rows.shape[0] // tall),
        in_specs=[pl.BlockSpec((tall, depth), lambda j, i: (i, 0))] + [piece] * len(pieces),
        out_specs=pl.BlockSpec((tall, wide), lambda j, i: (i, j)),
        out_shape=jax.ShapeDtypeStruct((rows.shape[0], width), jnp.bfloat16),
        cost_estimate=cost(2 * rows.size * width, rows, *pieces),
    )(rows, *pieces)


def broad_kernel(rows_ref, *refs):
    rows, out_ref = rows_ref[...], refs[-1]
    width = refs[0].shape[1]
    for place, ref in enumerate(refs[:-1]):
        out_ref[:, place * width : (place + 1) * width] = jnp.dot(
            rows, ref[...], preferred_element_type=jnp.float32
        ).astype(jnp.bfloat16)


def broad(rows, pieces):
    depth, width = pieces[0].shape
    tall = tile_of(rows.shape[0], 256)
    total = width * len(pieces)
    return pl.pallas_call(
        broad_kernel,
        grid=(rows.shape[0] // tall,),
        in_specs=[pl.BlockSpec((tall, depth), lambda i: (i, 0))]
        + [pl.BlockSpec((depth, width), lambda i: (0, 0))] * len(pieces),
        out_specs=pl.BlockSpec((tall, total), lambda i: (i, 0)),
        out_shape=jax.ShapeDtypeStruct((rows.shape[0], total), jnp.bfloat16),
        cost_estimate=cost(2 * rows.size * total, rows, *pieces),
    )(rows, *pieces)


def retain_kernel(decay_ref, query_ref, key_ref, value_ref, gain_ref, out_ref):
    head, block = pl.program_id(0), pl.program_id(1)
    tall, length = query_ref.shape[0], key_ref.shape[0]
    scores = lax.dot_general(
        query_ref[...], key_ref[...], (((1,), (1,)), ((), ())),
        preferred_element_type=jnp.float32,
    )
    here = lax.broadcasted_iota(jnp.int32, (tall, length), 0) + block * tall
    there = lax.broadcasted_iota(jnp.int32, (tall, length), 1)
    distance = (here - there).astype(jnp.float32)
    rate = jnp.where(distance >= 0, decay_ref[0, head], -decay_ref[1, head])
    decay = jnp.exp(rate * distance) * jnp.where(
        distance == 0, 2.0 * DK ** (-0.5), DK ** (-0.5)
    )
    outputs = jnp.dot(
        (scores * decay).astype(jnp.bfloat16), value_ref[...],
        preferred_element_type=jnp.float32,
    )
    centered = outputs - jnp.mean(outputs, axis=-1, keepdims=True)
    variance = jnp.mean(centered * centered, axis=-1, keepdims=True)
    out_ref[...] = (centered * lax.rsqrt(variance + EPS) * gain_ref[...]).astype(jnp.bfloat16)


def retain(queries, key_rows, value_rows, head_gain, log_decay):
    length, width = value_rows.shape
    tall = tile_of(length, 256)
    return pl.pallas_call(
        retain_kernel,
        grid=(width // DV, length // tall),
        in_specs=[
            pl.BlockSpec(memory_space=pltpu.SMEM),
            pl.BlockSpec((tall, DK), lambda h, i: (i, h)),
            pl.BlockSpec((length, DK), lambda h, i: (0, h)),
            pl.BlockSpec((length, DV), lambda h, i: (0, h)),
            pl.BlockSpec((1, DV), lambda h, i: (0, h)),
        ],
        out_specs=pl.BlockSpec((tall, DV), lambda h, i: (i, h)),
        out_shape=jax.ShapeDtypeStruct((length, width), jnp.bfloat16),
        cost_estimate=cost(3 * 2 * length * length * width // 2, queries, value_rows),
    )(log_decay, queries, key_rows, value_rows, head_gain.reshape(1, -1))


def chain_weight(weight, axis, size, group, after):
    me = lax.axis_index("fs")
    half = weight.shape[axis] // 2
    mine = lax.dynamic_slice_in_dim(weight, group * half, half, axis)
    other = lax.dynamic_slice_in_dim(weight, (1 - group) * half, half, axis)
    if after is not None:
        mine, _ = lax.optimization_barrier((mine, after))
    up_steps = [(i, i + 1) for i in range(size - 1)]
    down_steps = [(i + 1, i) for i in range(size - 1)]
    from_below, from_above = [mine], [mine]
    for _ in range(size - 1):
        from_below.append(lax.ppermute(from_below[-1], "fs", up_steps))
        from_above.append(lax.ppermute(from_above[-1], "fs", down_steps))
    pieces = [mine, other]
    for step in range(1, size):
        held = jnp.where(me + step < size, from_above[step], from_below[size - step])
        pieces += [held, lax.ppermute(held, "grp", [(0, 1), (1, 0)])]
    return pieces, (from_below[-1], from_above[-1])


def reorder(values, size, group, back):
    me = lax.axis_index("fs")
    half = values.shape[-1] // (2 * size)
    parts = []
    for place in range(2 * size):
        shard, side = place // 2, place % 2
        shard = lax.rem(shard - me + size, size) if back else lax.rem(shard + me, size)
        start = (2 * shard + jnp.bitwise_xor(side, group)) * half
        parts.append(lax.dynamic_slice_in_dim(values, start, half, values.ndim - 1))
    return jnp.concatenate(parts, axis=-1)


def shards_chained(
    size, tokens, first_gain, mixer_gain, gate_weight, up_weight, down_weight,
    query_weight, key_weight, value_weight, head_gain, out_weight, log_decay,
):
    group = lax.axis_index("grp")
    order = (
        (gate_weight, 0), (up_weight, 0), (down_weight, 1),
        (query_weight, 0), (key_weight, 0), (value_weight, 0), (out_weight, 1),
    )
    chained, ends = [], [None, None]
    for weight, axis in order:
        pieces, end = chain_weight(weight, axis, size, group, ends[-2])
        chained.append(pieces)
        ends.append(end)
    gates, ups, downs, querys, keys, values, outs = chained
    residual = reorder(tokens, size, group, False)
    normed = norm_rows(residual, reorder(first_gain, size, group, False))
    gathered = lax.all_gather(normed, "tp", axis=0, tiled=True)
    hidden = gated(gathered, gates, ups)
    summed = lax.psum_scatter(broad(hidden, downs), "tp", scatter_dimension=0, tiled=True)
    after_first = (
        residual.astype(jnp.float32) + 0.5 * summed.astype(jnp.float32)
    ).astype(jnp.bfloat16)
    normed = norm_rows(after_first, reorder(mixer_gain, size, group, False))
    gathered = lax.all_gather(normed, "tp", axis=0, tiled=True)
    flat = retain(
        deep(gathered, querys), deep(gathered, keys), deep(gathered, values),
        head_gain, log_decay,
    )
    summed = lax.psum_scatter(broad(flat, outs), "tp", scatter_dimension=0, tiled=True)
    updated = after_first.astype(jnp.float32) + summed.astype(jnp.float32)
    return reorder(updated.astype(jnp.bfloat16), size, group, True)


def shards_gathered(
    tokens, first_gain, mixer_gain, gate_weight, up_weight, down_weight,
    query_weight, key_weight, value_weight, head_gain, out_weight, log_decay,
):
    def rows_of(weight):
        return lax.all_gather(weight, "fs", axis=0, tiled=True)

    def columns_of(weight):
        return lax.all_gather(weight, "fs", axis=1, tiled=True)

    def times(left, right):
        return jnp.dot(left, right, preferred_element_type=jnp.float32)

    normed = norm_rows(tokens, first_gain)
    gathered = lax.all_gather(normed, "tp", axis=0, tiled=True)
    gate_sum = times(gathered, rows_of(gate_weight))
    hidden = (jax.nn.silu(gate_sum) * times(gathered, rows_of(up_weight))).astype(jnp.bfloat16)
    branch = times(hidden, columns_of(down_weight)).astype(jnp.bfloat16)
    summed = lax.psum_scatter(branch, "tp", scatter_dimension=0, tiled=True)
    after_first = (
        tokens.astype(jnp.float32) + 0.5 * summed.astype(jnp.float32)
    ).astype(jnp.bfloat16)
    gathered = lax.all_gather(norm_rows(after_first, mixer_gain), "tp", axis=0, tiled=True)
    queries, key_rows, value_rows = (
        times(gathered, rows_of(w)).astype(jnp.bfloat16)
        for w in (query_weight, key_weight, value_weight)
    )
    flat = retain(queries, key_rows, value_rows, head_gain, log_decay)
    branch = times(flat, columns_of(out_weight)).astype(jnp.bfloat16)
    summed = lax.psum_scatter(branch, "tp", scatter_dimension=0, tiled=True)
    return (after_first.astype(jnp.float32) + summed.astype(jnp.float32)).astype(jnp.bfloat16)


def shards(size, groups, *args):
    tokens = args[0]
    if groups == 2 and tokens.shape[1] % (2 * size * LANES) == 0:
        return shards_chained(size, *args)
    return shards_gathered(*args)


def solution(mesh):
    placed = (
        P(("grp", "fs", "tp"), None),
        P(),
        P(),
        P("fs", "tp"),
        P("fs", "tp"),
        P("tp", "fs"),
        P("fs", "tp"),
        P("fs", "tp"),
        P("fs", "tp"),
        P("tp"),
        P("tp", "fs"),
        P(None, "tp"),
    )
    return jax.shard_map(
        functools.partial(shards, mesh.shape["fs"], mesh.shape["grp"]),
        mesh=mesh, in_specs=placed, out_specs=P(("grp", "fs", "tp"), None), check_vma=False,
    )
```

```python
import functools

import jax
import jax.numpy as jnp
from jax import lax
from jax.experimental import pallas as pl
from jax.experimental.pallas import tpu as pltpu
from jax.sharding import PartitionSpec as P

DK = 256
DV = 512
EPS = 1e-06
LANES = 128


def norm_rows(values, gain):
    widened = values.astype(jnp.float32)
    factor = lax.rsqrt(jnp.mean(widened * widened, axis=-1, keepdims=True) + EPS)
    return (widened * factor * gain).astype(jnp.bfloat16)


def tile_of(width, top):
    best = width
    for tile in range(LANES, top + 1, LANES):
        if width % tile == 0:
            best = tile
    return best


def cost(flops, *arrays):
    return pl.CostEstimate(
        flops=flops,
        transcendentals=0,
        bytes_accessed=sum(a.size * a.dtype.itemsize for a in arrays),
    )


def retain_kernel(decay_ref, query_ref, key_ref, value_ref, gain_ref, out_ref):
    head, block = pl.program_id(0), pl.program_id(1)
    tall, length = query_ref.shape[0], key_ref.shape[0]
    scores = lax.dot_general(
        query_ref[...], key_ref[...], (((1,), (1,)), ((), ())),
        preferred_element_type=jnp.float32,
    )
    here = lax.broadcasted_iota(jnp.int32, (tall, length), 0) + block * tall
    there = lax.broadcasted_iota(jnp.int32, (tall, length), 1)
    distance = (here - there).astype(jnp.float32)
    rate = jnp.where(distance >= 0, decay_ref[0, head], -decay_ref[1, head])
    decay = jnp.exp(rate * distance) * jnp.where(
        distance == 0, 2.0 * DK ** (-0.5), DK ** (-0.5)
    )
    outputs = jnp.dot(
        (scores * decay).astype(jnp.bfloat16), value_ref[...],
        preferred_element_type=jnp.float32,
    )
    centered = outputs - jnp.mean(outputs, axis=-1, keepdims=True)
    variance = jnp.mean(centered * centered, axis=-1, keepdims=True)
    out_ref[...] = (centered * lax.rsqrt(variance + EPS) * gain_ref[...]).astype(jnp.bfloat16)


def retain(queries, key_rows, value_rows, head_gain, log_decay):
    length, width = value_rows.shape
    tall = tile_of(length, 256)
    return pl.pallas_call(
        retain_kernel,
        grid=(width // DV, length // tall),
        in_specs=[
            pl.BlockSpec(memory_space=pltpu.SMEM),
            pl.BlockSpec((tall, DK), lambda h, i: (i, h)),
            pl.BlockSpec((length, DK), lambda h, i: (0, h)),
            pl.BlockSpec((length, DV), lambda h, i: (0, h)),
            pl.BlockSpec((1, DV), lambda h, i: (0, h)),
        ],
        out_specs=pl.BlockSpec((tall, DV), lambda h, i: (i, h)),
        out_shape=jax.ShapeDtypeStruct((length, width), jnp.bfloat16),
        cost_estimate=cost(3 * 2 * length * length * width // 2, queries, value_rows),
    )(log_decay, queries, key_rows, value_rows, head_gain.reshape(1, -1))


def dot(left, right):
    return jnp.dot(left, right, preferred_element_type=jnp.float32)


def layer_kernel(size, *refs):
    (tokens, first_gain, mixer_gain, head_gain, decay) = refs[:5]
    sources, updated = refs[5:12], refs[12]
    weights = refs[13:20]
    (rows_one, rows_two, hidden, part, queries, key_rows, value_rows, flat, after_first,
     far_one, near_one, cross_one, pair_one, far_two, near_two, cross_two, pair_two,
     local_sem, z_recv, z_send, z_left, y_recv, y_send, tp_send, tp_recv) = refs[20:]
    gate, up, down, query_w, key_w, value_w, out_w = weights
    column_split = (False, False, True, False, False, False, True)
    group, z, spot = lax.axis_index("grp"), lax.axis_index("fs"), lax.axis_index("tp")
    chip, core = spot // 2, spot % 2
    mate = chip * 2 + (1 - core)
    peer = (1 - chip) * 2 + core
    last = size - 1
    band = tokens.shape[0]

    def shard_at(w, shard, side=None):
        tall, wide = sources[w].shape
        height = tall if side is None else tall // 2
        start = 0 if side is None else side * height
        if column_split[w]:
            return weights[w].at[
                pl.ds(pl.multiple_of(start, height), height),
                pl.ds(pl.multiple_of(shard * wide, wide), wide),
            ]
        return weights[w].at[pl.ds(pl.multiple_of(shard * tall + start, height), height), :]

    def own_copy(w):
        return pltpu.make_async_copy(sources[w], shard_at(w, z), local_sem.at[w])

    def along(w, shard, to, send_sem):
        block = shard_at(w, shard, group)
        return pltpu.make_async_remote_copy(
            src_ref=block, dst_ref=block, send_sem=send_sem, recv_sem=z_recv.at[w, shard],
            device_id={"fs": to}, device_id_type=pl.DeviceIdType.MESH,
        )

    def across(w, shard, side):
        block = shard_at(w, shard, side)
        return pltpu.make_async_remote_copy(
            src_ref=block, dst_ref=block, send_sem=y_send.at[w, shard],
            recv_sem=y_recv.at[w, shard],
            device_id={"grp": 1 - group}, device_id_type=pl.DeviceIdType.MESH,
        )

    def send_tp(source, target, number, to):
        return pltpu.make_async_remote_copy(
            src_ref=source, dst_ref=target, send_sem=tp_send.at[number],
            recv_sem=tp_recv.at[number],
            device_id={"tp": to}, device_id_type=pl.DeviceIdType.MESH,
        )

    def start(w):
        own_copy(w).wait()

        @pl.when(z < last)
        def _():
            along(w, z, z + 1, z_send.at[w, z]).start()

        @pl.when(z > 0)
        def _():
            along(w, z, z - 1, z_left.at[w]).start()

    def step(w, k):
        @pl.when(z - k >= 0)
        def _():
            copy = along(w, z - k, z + 1, z_send.at[w, z - k])
            copy.wait_recv()

            @pl.when(z < last)
            def _():
                copy.start()

            across(w, z - k, group).start()

        @pl.when(z + k <= last)
        def _():
            copy = along(w, z + k, z - 1, z_send.at[w, z + k])
            copy.wait_recv()

            @pl.when(z > 0)
            def _():
                copy.start()

            across(w, z + k, group).start()

    def steps(w):
        for k in range(1, size):
            step(w, k)

    def finish(w):
        for k in range(1, size):
            @pl.when(z - k >= 0)
            def _():
                across(w, z - k, 1 - group).wait_recv()

            @pl.when(z + k <= last)
            def _():
                across(w, z + k, 1 - group).wait_recv()

    def drain(w):
        @pl.when(z < last)
        def _():
            along(w, z, z + 1, z_send.at[w, z]).wait_send()

        @pl.when(z > 0)
        def _():
            along(w, z, z - 1, z_left.at[w]).wait_send()

        for k in range(1, size):
            @pl.when(z - k >= 0)
            def _():
                @pl.when(z < last)
                def _():
                    along(w, z - k, z + 1, z_send.at[w, z - k]).wait_send()

                across(w, z - k, group).wait_send()

            @pl.when(z + k <= last)
            def _():
                @pl.when(z > 0)
                def _():
                    along(w, z + k, z - 1, z_send.at[w, z + k]).wait_send()

                across(w, z + k, group).wait_send()

    def band_of(ref, place):
        return ref.at[pl.ds(pl.multiple_of(place * band, band), band), :]

    def by_chunks(body):
        tall = band // 4

        def chunk(i, carry):
            body(pl.multiple_of(i * tall, tall), tall)
            return carry

        lax.fori_loop(0, 4, chunk, 0)

    def normed_into(rows, source, gain):
        def body(first, tall):
            start_row = pl.multiple_of(spot * band + first, tall)
            rows[pl.ds(start_row, tall), :] = norm_rows(source[pl.ds(first, tall), :], gain[...])

        by_chunks(body)

    def gather_start(rows, base):
        mine = band_of(rows, spot)
        send_tp(mine, mine, base + 1, peer).start()
        send_tp(mine, mine, base, mate).start()

    def gather_forward(rows, base):
        theirs = band_of(rows, peer)
        send_tp(theirs, theirs, base + 1, peer).wait_recv()
        send_tp(theirs, theirs, base + 2, mate).start()

    def gather_end(rows, base):
        near, beyond = band_of(rows, mate), band_of(rows, (1 - chip) * 2 + (1 - core))
        send_tp(near, near, base, mate).wait_recv()
        send_tp(beyond, beyond, base + 2, mate).wait_recv()

    def gather_drain(rows, base):
        for number, to in ((0, mate), (1, peer), (2, mate)):
            send_tp(band_of(rows, spot), band_of(rows, spot), base + number, to).wait_send()

    def product(target, source, weight, first, tall, wide):
        def tile(t, carry):
            columns = pl.ds(pl.multiple_of(t * wide, wide), wide)
            target[pl.ds(first, tall), columns] = dot(
                source[pl.ds(first, tall), :], weight[:, columns]
            ).astype(jnp.bfloat16)
            return carry

        lax.fori_loop(0, weight.shape[1] // wide, tile, 0)

    def scatter_far(far, base):
        send_tp(band_of(part, (1 - chip) * 2 + (1 - core)), far, base, mate).start()

    def scatter_near(near, base):
        send_tp(band_of(part, mate), near, base + 1, mate).start()

    def scatter_cross(far, pair, cross, base):
        send_tp(far, far, base, mate).wait_recv()

        def body(first, tall):
            from_row = pl.multiple_of(peer * band + first, tall)
            pair[pl.ds(first, tall), :] = (
                part[pl.ds(from_row, tall), :].astype(jnp.float32)
                + far[pl.ds(first, tall), :].astype(jnp.float32)
            ).astype(jnp.bfloat16)

        by_chunks(body)
        send_tp(pair, cross, base + 2, peer).start()

    def scatter_end(residual, near, cross, scale, target, base):
        send_tp(near, near, base + 1, mate).wait_recv()
        send_tp(cross, cross, base + 2, peer).wait_recv()

        def body(first, tall):
            here = pl.ds(first, tall)
            own_row = pl.multiple_of(spot * band + first, tall)
            total = part[pl.ds(own_row, tall), :].astype(jnp.float32)
            total = total + near[here, :].astype(jnp.float32)
            total = total + cross[here, :].astype(jnp.float32)
            target[here, :] = (
                residual[here, :].astype(jnp.float32) + scale * total
            ).astype(jnp.bfloat16)

        by_chunks(body)

    def scatter_drain(near, base):
        for number, to in ((0, mate), (1, mate), (2, peer)):
            send_tp(near, near, base + number, to).wait_send()

    half_rows = 2 * band
    far_rows = pl.multiple_of((1 - chip) * half_rows, half_rows)
    chip_rows = pl.multiple_of(chip * half_rows, half_rows)

    def gated_rows(first):
        wide = tile_of(gate.shape[1], 384)

        def tile(t, carry):
            columns = pl.ds(pl.multiple_of(t * wide, LANES), wide)
            rows = rows_one[pl.ds(first, half_rows), :]
            gate_sum = dot(rows, gate[:, columns])
            up_sum = dot(rows, up[:, columns])
            hidden[pl.ds(first, half_rows), columns] = (
                gate_sum / (1.0 + jnp.exp(-gate_sum)) * up_sum
            ).astype(jnp.bfloat16)
            return carry

        lax.fori_loop(0, gate.shape[1] // wide, tile, 0)

    def retain_head(head):
        length = key_rows.shape[0]
        tall = tile_of(length, 256)
        keyed = slice(head * DK, (head + 1) * DK)
        valued = slice(head * DV, (head + 1) * DV)

        def tile(i, carry):
            first = pl.multiple_of(i * tall, tall)
            scores = lax.dot_general(
                queries[pl.ds(first, tall), keyed], key_rows[:, keyed],
                (((1,), (1,)), ((), ())), preferred_element_type=jnp.float32,
            )
            here = lax.broadcasted_iota(jnp.int32, (tall, length), 0) + first
            there = lax.broadcasted_iota(jnp.int32, (tall, length), 1)
            distance = (here - there).astype(jnp.float32)
            rate = jnp.where(distance >= 0, decay[0, head], -decay[1, head])
            factor = jnp.where(distance == 0, 2.0 * DK ** (-0.5), DK ** (-0.5))
            weighted = (scores * (jnp.exp(rate * distance) * factor)).astype(jnp.bfloat16)
            outputs = dot(weighted, value_rows[:, valued])
            centered = outputs - jnp.mean(outputs, axis=-1, keepdims=True)
            variance = jnp.mean(centered * centered, axis=-1, keepdims=True)
            flat[pl.ds(first, tall), valued] = (
                centered * lax.rsqrt(variance + EPS) * head_gain[:, valued]
            ).astype(jnp.bfloat16)
            return carry

        lax.fori_loop(0, length // tall, tile, 0)

    for w in range(7):
        own_copy(w).start()
    barrier = pltpu.get_barrier_semaphore()

    def greet(**where):
        pl.semaphore_signal(
            barrier, inc=1, device_id=where, device_id_type=pl.DeviceIdType.MESH
        )

    greet(tp=mate)
    greet(tp=peer)
    greet(grp=1 - group)

    @pl.when(z > 0)
    def _():
        greet(fs=z - 1)

    @pl.when(z < last)
    def _():
        greet(fs=z + 1)

    pl.semaphore_wait(barrier, 3 + jnp.minimum(z, 1) + jnp.minimum(last - z, 1))

    start(0)
    start(1)
    normed_into(rows_one, tokens, first_gain)
    gather_start(rows_one, 0)
    step(0, 1)
    start(2)
    for k in range(2, size):
        step(0, k)
    gather_forward(rows_one, 0)
    step(1, 1)
    start(3)
    for k in range(2, size):
        step(1, k)
    gather_end(rows_one, 0)
    finish(0)
    step(2, 1)
    start(4)
    finish(1)
    gated_rows(0)
    step(2, 2)
    gated_rows(half_rows)
    for k in range(3, size):
        step(2, k)
    step(3, 1)
    start(5)
    finish(2)
    product(part, hidden, down, far_rows, half_rows, 512)
    scatter_far(far_one, 3)
    product(part, hidden, down, chip_rows, half_rows, 512)
    scatter_near(near_one, 3)
    scatter_cross(far_one, pair_one, cross_one, 3)
    for k in range(2, size):
        step(3, k)
    scatter_end(tokens, near_one, cross_one, 0.5, after_first, 3)
    normed_into(rows_two, after_first, mixer_gain)
    gather_start(rows_two, 6)
    step(4, 1)
    start(6)
    for k in range(2, size):
        step(4, k)
    step(5, 1)
    gather_forward(rows_two, 6)
    step(5, 2)
    gather_end(rows_two, 6)
    finish(3)
    for first in (0, half_rows):
        product(queries, rows_two, query_w, first, half_rows, 512)
    for k in range(3, size):
        step(5, k)
    step(6, 1)
    finish(4)
    for first in (0, half_rows):
        product(key_rows, rows_two, key_w, first, half_rows, 512)
    finish(5)
    product(value_rows, rows_two, value_w, 0, half_rows, 512)
    step(6, 2)
    product(value_rows, rows_two, value_w, half_rows, half_rows, 512)
    for k in range(3, size):
        step(6, k)
    for head in range(value_rows.shape[1] // DV):
        retain_head(head)
    finish(6)
    scatter_drain(near_one, 3)
    product(part, flat, out_w, far_rows, half_rows, 512)
    scatter_far(far_two, 9)
    product(part, flat, out_w, chip_rows, half_rows, 512)
    scatter_near(near_two, 9)
    scatter_cross(far_two, pair_two, cross_two, 9)
    scatter_end(after_first, near_two, cross_two, 1.0, updated, 9)
    for w in range(7):
        drain(w)
    gather_drain(rows_one, 0)
    gather_drain(rows_two, 6)
    scatter_drain(near_two, 9)


def shards_fused(
    size, tokens, first_gain, mixer_gain, gate_weight, up_weight, down_weight,
    query_weight, key_weight, value_weight, head_gain, out_weight, log_decay,
):
    band, depth = tokens.shape
    length = 4 * band
    sources = (
        gate_weight, up_weight, down_weight, query_weight, key_weight, value_weight, out_weight
    )

    def held(*shape):
        return pltpu.VMEM(shape, jnp.bfloat16)

    whole = [
        held(w.shape[0], w.shape[1] * size) if place in (2, 6) else held(w.shape[0] * size, w.shape[1])
        for place, w in enumerate(sources)
    ]
    dma = pltpu.SemaphoreType.DMA
    count = len(sources)
    in_vmem = pl.BlockSpec(memory_space=pltpu.VMEM)
    return pl.pallas_call(
        functools.partial(layer_kernel, size),
        in_specs=[in_vmem] * 4
        + [pl.BlockSpec(memory_space=pltpu.SMEM)]
        + [pl.BlockSpec(memory_space=pl.ANY)] * count,
        out_specs=in_vmem,
        out_shape=jax.ShapeDtypeStruct(tokens.shape, tokens.dtype),
        scratch_shapes=whole
        + [
            held(length, depth), held(length, depth), held(length, gate_weight.shape[1]),
            held(length, depth), held(length, query_weight.shape[1]),
            held(length, key_weight.shape[1]), held(length, value_weight.shape[1]),
            held(length, value_weight.shape[1]), held(band, depth),
        ]
        + [held(band, depth)] * 8
        + [
            dma((count,)), dma((count, size)), dma((count, size)), dma((count,)),
            dma((count, size)), dma((count, size)), dma((12,)), dma((12,)),
        ],
        compiler_params=pltpu.CompilerParams(
            collective_id=0, has_side_effects=True, vmem_limit_bytes=67_000_000
        ),
    )(
        tokens, first_gain.reshape(1, -1), mixer_gain.reshape(1, -1), head_gain.reshape(1, -1),
        log_decay, *sources,
    )


def shards_gathered(
    tokens, first_gain, mixer_gain, gate_weight, up_weight, down_weight,
    query_weight, key_weight, value_weight, head_gain, out_weight, log_decay,
):
    def rows_of(weight):
        return lax.all_gather(weight, "fs", axis=0, tiled=True)

    def columns_of(weight):
        return lax.all_gather(weight, "fs", axis=1, tiled=True)

    def times(left, right):
        return jnp.dot(left, right, preferred_element_type=jnp.float32)

    normed = norm_rows(tokens, first_gain)
    gathered = lax.all_gather(normed, "tp", axis=0, tiled=True)
    gate_sum = times(gathered, rows_of(gate_weight))
    hidden = (jax.nn.silu(gate_sum) * times(gathered, rows_of(up_weight))).astype(jnp.bfloat16)
    branch = times(hidden, columns_of(down_weight)).astype(jnp.bfloat16)
    summed = lax.psum_scatter(branch, "tp", scatter_dimension=0, tiled=True)
    after_first = (
        tokens.astype(jnp.float32) + 0.5 * summed.astype(jnp.float32)
    ).astype(jnp.bfloat16)
    gathered = lax.all_gather(norm_rows(after_first, mixer_gain), "tp", axis=0, tiled=True)
    queries, key_rows, value_rows = (
        times(gathered, rows_of(w)).astype(jnp.bfloat16)
        for w in (query_weight, key_weight, value_weight)
    )
    flat = retain(queries, key_rows, value_rows, head_gain, log_decay)
    branch = times(flat, columns_of(out_weight)).astype(jnp.bfloat16)
    summed = lax.psum_scatter(branch, "tp", scatter_dimension=0, tiled=True)
    return (after_first.astype(jnp.float32) + summed.astype(jnp.float32)).astype(jnp.bfloat16)


def shards(sizes, *args):
    depth = args[3].shape[0] * sizes["fs"]
    if sizes["grp"] == 2 and sizes["tp"] == 4 and depth % (2 * sizes["fs"] * LANES) == 0:
        return shards_fused(sizes["fs"], *args)
    return shards_gathered(*args)


def solution(mesh):
    placed = (
        P(("grp", "fs", "tp"), None),
        P(),
        P(),
        P("fs", "tp"),
        P("fs", "tp"),
        P("tp", "fs"),
        P("fs", "tp"),
        P("fs", "tp"),
        P("fs", "tp"),
        P("tp"),
        P("tp", "fs"),
        P(None, "tp"),
    )
    return jax.shard_map(
        functools.partial(shards, dict(mesh.shape)),
        mesh=mesh, in_specs=placed, out_specs=P(("grp", "fs", "tp"), None), check_vma=False,
    )
```

```python
import functools

import jax
import jax.numpy as jnp
from jax import lax
from jax.experimental import pallas as pl
from jax.experimental.pallas import tpu as pltpu
from jax.sharding import PartitionSpec as P

DK = 256
DV = 512
EPS = 1e-06
LANES = 128


def norm_rows(values, gain):
    widened = values.astype(jnp.float32)
    factor = lax.rsqrt(jnp.mean(widened * widened, axis=-1, keepdims=True) + EPS)
    return (widened * factor * gain).astype(jnp.bfloat16)


def tile_of(width, top):
    best = width
    for tile in range(LANES, top + 1, LANES):
        if width % tile == 0:
            best = tile
    return best


def cost(flops, *arrays):
    return pl.CostEstimate(
        flops=flops,
        transcendentals=0,
        bytes_accessed=sum(a.size * a.dtype.itemsize for a in arrays),
    )


def retain_kernel(decay_ref, query_ref, key_ref, value_ref, gain_ref, out_ref):
    head, block = pl.program_id(0), pl.program_id(1)
    tall, length = query_ref.shape[0], key_ref.shape[0]
    scores = lax.dot_general(
        query_ref[...], key_ref[...], (((1,), (1,)), ((), ())),
        preferred_element_type=jnp.float32,
    )
    here = lax.broadcasted_iota(jnp.int32, (tall, length), 0) + block * tall
    there = lax.broadcasted_iota(jnp.int32, (tall, length), 1)
    distance = (here - there).astype(jnp.float32)
    rate = jnp.where(distance >= 0, decay_ref[0, head], -decay_ref[1, head])
    decay = jnp.exp(rate * distance) * jnp.where(
        distance == 0, 2.0 * DK ** (-0.5), DK ** (-0.5)
    )
    outputs = jnp.dot(
        (scores * decay).astype(jnp.bfloat16), value_ref[...],
        preferred_element_type=jnp.float32,
    )
    centered = outputs - jnp.mean(outputs, axis=-1, keepdims=True)
    variance = jnp.mean(centered * centered, axis=-1, keepdims=True)
    out_ref[...] = (centered * lax.rsqrt(variance + EPS) * gain_ref[...]).astype(jnp.bfloat16)


def retain(queries, key_rows, value_rows, head_gain, log_decay):
    length, width = value_rows.shape
    tall = tile_of(length, 256)
    return pl.pallas_call(
        retain_kernel,
        grid=(width // DV, length // tall),
        in_specs=[
            pl.BlockSpec(memory_space=pltpu.SMEM),
            pl.BlockSpec((tall, DK), lambda h, i: (i, h)),
            pl.BlockSpec((length, DK), lambda h, i: (0, h)),
            pl.BlockSpec((length, DV), lambda h, i: (0, h)),
            pl.BlockSpec((1, DV), lambda h, i: (0, h)),
        ],
        out_specs=pl.BlockSpec((tall, DV), lambda h, i: (i, h)),
        out_shape=jax.ShapeDtypeStruct((length, width), jnp.bfloat16),
        cost_estimate=cost(3 * 2 * length * length * width // 2, queries, value_rows),
    )(log_decay, queries, key_rows, value_rows, head_gain.reshape(1, -1))


def dot(left, right):
    return jnp.dot(left, right, preferred_element_type=jnp.float32)


def layer_kernel(size, *refs):
    (tokens, first_gain, mixer_gain, head_gain, decay) = refs[:5]
    sources, updated = refs[5:12], refs[12]
    weights = refs[13:20]
    (rows_one, rows_two, hidden, part, queries, key_rows, value_rows, flat, after_first,
     far_one, near_one, cross_one, pair_one, far_two, near_two, cross_two, pair_two,
     local_sem, z_recv, z_send, z_left, y_recv, y_send, tp_send, tp_recv) = refs[20:]
    gate, up, down, query_w, key_w, value_w, out_w = weights
    column_split = (False, False, True, False, False, False, True)
    group, z, spot = lax.axis_index("grp"), lax.axis_index("fs"), lax.axis_index("tp")
    chip, core = spot // 2, spot % 2
    mate = chip * 2 + (1 - core)
    peer = (1 - chip) * 2 + core
    last = size - 1
    band = tokens.shape[0]

    def shard_at(w, shard, side=None):
        tall, wide = sources[w].shape
        height = tall if side is None else tall // 2
        start = 0 if side is None else side * height
        if column_split[w]:
            return weights[w].at[
                pl.ds(pl.multiple_of(start, height), height),
                pl.ds(pl.multiple_of(shard * wide, wide), wide),
            ]
        return weights[w].at[pl.ds(pl.multiple_of(shard * tall + start, height), height), :]

    def own_copy(w):
        return pltpu.make_async_copy(sources[w], shard_at(w, z), local_sem.at[w])

    def along(w, shard, to, send_sem):
        block = shard_at(w, shard, group)
        return pltpu.make_async_remote_copy(
            src_ref=block, dst_ref=block, send_sem=send_sem, recv_sem=z_recv.at[w, shard],
            device_id={"fs": to}, device_id_type=pl.DeviceIdType.MESH,
        )

    def across(w, shard, side):
        block = shard_at(w, shard, side)
        return pltpu.make_async_remote_copy(
            src_ref=block, dst_ref=block, send_sem=y_send.at[w, shard],
            recv_sem=y_recv.at[w, shard],
            device_id={"grp": 1 - group}, device_id_type=pl.DeviceIdType.MESH,
        )

    def send_tp(source, target, number, to):
        return pltpu.make_async_remote_copy(
            src_ref=source, dst_ref=target, send_sem=tp_send.at[number],
            recv_sem=tp_recv.at[number],
            device_id={"tp": to}, device_id_type=pl.DeviceIdType.MESH,
        )

    def start(w):
        own_copy(w).wait()

        @pl.when(z < last)
        def _():
            along(w, z, z + 1, z_send.at[w, z]).start()

        @pl.when(z > 0)
        def _():
            along(w, z, z - 1, z_left.at[w]).start()

    def step(w, k):
        @pl.when(z - k >= 0)
        def _():
            copy = along(w, z - k, z + 1, z_send.at[w, z - k])
            copy.wait_recv()

            @pl.when(z < last)
            def _():
                copy.start()

            across(w, z - k, group).start()

        @pl.when(z + k <= last)
        def _():
            copy = along(w, z + k, z - 1, z_send.at[w, z + k])
            copy.wait_recv()

            @pl.when(z > 0)
            def _():
                copy.start()

            across(w, z + k, group).start()

    def steps(w):
        for k in range(1, size):
            step(w, k)

    def finish(w):
        for k in range(1, size):
            @pl.when(z - k >= 0)
            def _():
                across(w, z - k, 1 - group).wait_recv()

            @pl.when(z + k <= last)
            def _():
                across(w, z + k, 1 - group).wait_recv()

    def arrival(place):
        order = [sorted(range(size), key=lambda s: (abs(s - here), s)) for here in range(size)]
        return sum(jnp.where(z == here, order[here][place], 0) for here in range(size))

    def finish_shard(w, shard):
        across(w, shard, 1 - group).wait_recv()

    def drain(w):
        @pl.when(z < last)
        def _():
            along(w, z, z + 1, z_send.at[w, z]).wait_send()

        @pl.when(z > 0)
        def _():
            along(w, z, z - 1, z_left.at[w]).wait_send()

        for k in range(1, size):
            @pl.when(z - k >= 0)
            def _():
                @pl.when(z < last)
                def _():
                    along(w, z - k, z + 1, z_send.at[w, z - k]).wait_send()

                across(w, z - k, group).wait_send()

            @pl.when(z + k <= last)
            def _():
                @pl.when(z > 0)
                def _():
                    along(w, z + k, z - 1, z_send.at[w, z + k]).wait_send()

                across(w, z + k, group).wait_send()

    def band_of(ref, place):
        return ref.at[pl.ds(pl.multiple_of(place * band, band), band), :]

    def by_chunks(body):
        tall = band // 4

        def chunk(i, carry):
            body(pl.multiple_of(i * tall, tall), tall)
            return carry

        lax.fori_loop(0, 4, chunk, 0)

    def normed_into(rows, source, gain):
        def body(first, tall):
            start_row = pl.multiple_of(spot * band + first, tall)
            rows[pl.ds(start_row, tall), :] = norm_rows(source[pl.ds(first, tall), :], gain[...])

        by_chunks(body)

    def gather_start(rows, base):
        mine = band_of(rows, spot)
        send_tp(mine, mine, base + 1, peer).start()
        send_tp(mine, mine, base, mate).start()

    def gather_forward(rows, base):
        theirs = band_of(rows, peer)
        send_tp(theirs, theirs, base + 1, peer).wait_recv()
        send_tp(theirs, theirs, base + 2, mate).start()

    def gather_end(rows, base):
        near, beyond = band_of(rows, mate), band_of(rows, (1 - chip) * 2 + (1 - core))
        send_tp(near, near, base, mate).wait_recv()
        send_tp(beyond, beyond, base + 2, mate).wait_recv()

    def gather_drain(rows, base):
        for number, to in ((0, mate), (1, peer), (2, mate)):
            send_tp(band_of(rows, spot), band_of(rows, spot), base + number, to).wait_send()

    def product(target, source, weight, first, tall, wide):
        def tile(t, carry):
            columns = pl.ds(pl.multiple_of(t * wide, wide), wide)
            target[pl.ds(first, tall), columns] = dot(
                source[pl.ds(first, tall), :], weight[:, columns]
            ).astype(jnp.bfloat16)
            return carry

        lax.fori_loop(0, weight.shape[1] // wide, tile, 0)

    stripe = tokens.shape[1] // size

    def columns_of(shard):
        return pl.ds(pl.multiple_of(shard * stripe, stripe), stripe)

    def band_part(ref, place, shard):
        return ref.at[pl.ds(pl.multiple_of(place * band, band), band), columns_of(shard)]

    def stripe_of(ref, shard):
        return ref.at[:, columns_of(shard)]

    def scatter_stripe(source, weight, buffers, base, place):
        far, near = buffers[:2]
        shard = arrival(place)
        columns = columns_of(shard)
        for first in (far_rows, chip_rows):
            there = pl.ds(first, half_rows)
            part[there, columns] = dot(source[there, :], weight[:, columns]).astype(jnp.bfloat16)
        beyond = (1 - chip) * 2 + (1 - core)
        send_tp(
            band_part(part, beyond, shard), stripe_of(far, shard), base + place, mate
        ).start()
        send_tp(
            band_part(part, mate, shard), stripe_of(near, shard), base + size + place, mate
        ).start()

    def scatter_cross(buffers, base, place):
        far, near, cross, pair = buffers
        shard = arrival(place)
        columns = columns_of(shard)
        block = stripe_of(far, shard)
        send_tp(block, block, base + place, mate).wait_recv()

        def body(first, tall):
            from_row = pl.multiple_of(peer * band + first, tall)
            pair[pl.ds(first, tall), columns] = (
                part[pl.ds(from_row, tall), columns].astype(jnp.float32)
                + far[pl.ds(first, tall), columns].astype(jnp.float32)
            ).astype(jnp.bfloat16)

        by_chunks(body)
        send_tp(
            stripe_of(pair, shard), stripe_of(cross, shard), base + 2 * size + place, peer
        ).start()

    def scatter_end(residual, buffers, scale, target, base):
        far, near, cross, pair = buffers
        for place in range(size):
            shard = arrival(place)
            columns = columns_of(shard)
            block, peer_block = stripe_of(near, shard), stripe_of(cross, shard)
            send_tp(block, block, base + size + place, mate).wait_recv()
            send_tp(peer_block, peer_block, base + 2 * size + place, peer).wait_recv()

            def body(first, tall):
                here = pl.ds(first, tall)
                own_row = pl.multiple_of(spot * band + first, tall)
                total = part[pl.ds(own_row, tall), columns].astype(jnp.float32)
                total = total + near[here, columns].astype(jnp.float32)
                total = total + cross[here, columns].astype(jnp.float32)
                target[here, columns] = (
                    residual[here, columns].astype(jnp.float32) + scale * total
                ).astype(jnp.bfloat16)

            by_chunks(body)

    def scatter_drain(buffers, base):
        for number in range(3 * size):
            block = stripe_of(buffers[1], 0)
            to = peer if number >= 2 * size else mate
            send_tp(block, block, base + number, to).wait_send()

    one, two = (far_one, near_one, cross_one, pair_one), (far_two, near_two, cross_two, pair_two)
    half_rows = 2 * band
    far_rows = pl.multiple_of((1 - chip) * half_rows, half_rows)
    chip_rows = pl.multiple_of(chip * half_rows, half_rows)

    def gated_rows(first):
        wide = tile_of(gate.shape[1], 384)

        def tile(t, carry):
            columns = pl.ds(pl.multiple_of(t * wide, LANES), wide)
            rows = rows_one[pl.ds(first, half_rows), :]
            gate_sum = dot(rows, gate[:, columns])
            up_sum = dot(rows, up[:, columns])
            hidden[pl.ds(first, half_rows), columns] = (
                gate_sum / (1.0 + jnp.exp(-gate_sum)) * up_sum
            ).astype(jnp.bfloat16)
            return carry

        lax.fori_loop(0, gate.shape[1] // wide, tile, 0)

    def retain_head(head):
        length = key_rows.shape[0]
        tall = tile_of(length, 256)
        keyed = slice(head * DK, (head + 1) * DK)
        valued = slice(head * DV, (head + 1) * DV)

        def tile(i, carry):
            first = pl.multiple_of(i * tall, tall)
            scores = lax.dot_general(
                queries[pl.ds(first, tall), keyed], key_rows[:, keyed],
                (((1,), (1,)), ((), ())), preferred_element_type=jnp.float32,
            )
            here = lax.broadcasted_iota(jnp.int32, (tall, length), 0) + first
            there = lax.broadcasted_iota(jnp.int32, (tall, length), 1)
            distance = (here - there).astype(jnp.float32)
            rate = jnp.where(distance >= 0, decay[0, head], -decay[1, head])
            factor = jnp.where(distance == 0, 2.0 * DK ** (-0.5), DK ** (-0.5))
            weighted = (scores * (jnp.exp(rate * distance) * factor)).astype(jnp.bfloat16)
            outputs = dot(weighted, value_rows[:, valued])
            centered = outputs - jnp.mean(outputs, axis=-1, keepdims=True)
            variance = jnp.mean(centered * centered, axis=-1, keepdims=True)
            flat[pl.ds(first, tall), valued] = (
                centered * lax.rsqrt(variance + EPS) * head_gain[:, valued]
            ).astype(jnp.bfloat16)
            return carry

        lax.fori_loop(0, length // tall, tile, 0)

    for w in range(7):
        own_copy(w).start()
    barrier = pltpu.get_barrier_semaphore()

    def greet(**where):
        pl.semaphore_signal(
            barrier, inc=1, device_id=where, device_id_type=pl.DeviceIdType.MESH
        )

    greet(tp=mate)
    greet(tp=peer)
    greet(grp=1 - group)

    @pl.when(z > 0)
    def _():
        greet(fs=z - 1)

    @pl.when(z < last)
    def _():
        greet(fs=z + 1)

    pl.semaphore_wait(barrier, 3 + jnp.minimum(z, 1) + jnp.minimum(last - z, 1))

    def pump(t):
        for k in range(1, size):
            w = t - k + 1
            if 0 <= w < 7:
                step(w, k)
            if k == 1 and t + 2 < 7:
                start(t + 2)

    start(0)
    start(1)
    normed_into(rows_one, tokens, first_gain)
    gather_start(rows_one, 0)
    pump(0)
    pump(1)
    gather_forward(rows_one, 0)
    for t in range(2, size):
        pump(t)
    gather_end(rows_one, 0)
    finish(0)
    pump(size)
    finish(1)
    gated_rows(0)
    step(5, 1)
    gated_rows(half_rows)
    scatter_stripe(hidden, down, one, 6, 0)
    for k in range(2, size):
        step(6 - k, k)
    finish_shard(2, arrival(1))
    scatter_stripe(hidden, down, one, 6, 1)
    scatter_cross(one, 6, 0)
    for place in range(2, size):
        finish_shard(2, arrival(place))
        scatter_stripe(hidden, down, one, 6, place)
        scatter_cross(one, 6, place - 1)
    scatter_cross(one, 6, size - 1)
    step(6, 1)
    step(5, 2)
    scatter_end(tokens, one, 0.5, after_first, 6)
    normed_into(rows_two, after_first, mixer_gain)
    gather_start(rows_two, 3)
    for k in range(3, size):
        step(7 - k, k)
    pump(7)
    gather_forward(rows_two, 3)
    for t in range(8, 5 + size):
        pump(t)
    gather_end(rows_two, 3)
    finish(3)
    for first in (0, half_rows):
        product(queries, rows_two, query_w, first, half_rows, 512)
    finish(4)
    for first in (0, half_rows):
        product(key_rows, rows_two, key_w, first, half_rows, 512)
    finish(5)
    for first in (0, half_rows):
        product(value_rows, rows_two, value_w, first, half_rows, 512)
    for head in range(value_rows.shape[1] // DV):
        retain_head(head)
    scatter_drain(one, 6)
    scatter_stripe(flat, out_w, two, 6 + 3 * size, 0)
    for place in range(1, size):
        finish_shard(6, arrival(place))
        scatter_stripe(flat, out_w, two, 6 + 3 * size, place)
        scatter_cross(two, 6 + 3 * size, place - 1)
    scatter_cross(two, 6 + 3 * size, size - 1)
    scatter_end(after_first, two, 1.0, updated, 6 + 3 * size)
    for w in range(7):
        drain(w)
    gather_drain(rows_one, 0)
    gather_drain(rows_two, 3)
    scatter_drain(two, 6 + 3 * size)


def shards_fused(
    size, tokens, first_gain, mixer_gain, gate_weight, up_weight, down_weight,
    query_weight, key_weight, value_weight, head_gain, out_weight, log_decay,
):
    band, depth = tokens.shape
    length = 4 * band
    sources = (
        gate_weight, up_weight, down_weight, query_weight, key_weight, value_weight, out_weight
    )

    def held(*shape):
        return pltpu.VMEM(shape, jnp.bfloat16)

    whole = [
        held(w.shape[0], w.shape[1] * size) if place in (2, 6) else held(w.shape[0] * size, w.shape[1])
        for place, w in enumerate(sources)
    ]
    dma = pltpu.SemaphoreType.DMA
    count = len(sources)
    in_vmem = pl.BlockSpec(memory_space=pltpu.VMEM)
    return pl.pallas_call(
        functools.partial(layer_kernel, size),
        in_specs=[in_vmem] * 4
        + [pl.BlockSpec(memory_space=pltpu.SMEM)]
        + [pl.BlockSpec(memory_space=pl.ANY)] * count,
        out_specs=in_vmem,
        out_shape=jax.ShapeDtypeStruct(tokens.shape, tokens.dtype),
        scratch_shapes=whole
        + [
            held(length, depth), held(length, depth), held(length, gate_weight.shape[1]),
            held(length, depth), held(length, query_weight.shape[1]),
            held(length, key_weight.shape[1]), held(length, value_weight.shape[1]),
            held(length, value_weight.shape[1]), held(band, depth),
        ]
        + [held(band, depth)] * 8
        + [
            dma((count,)), dma((count, size)), dma((count, size)), dma((count,)),
            dma((count, size)), dma((count, size)), dma((6 + 6 * size,)), dma((6 + 6 * size,)),
        ],
        compiler_params=pltpu.CompilerParams(
            collective_id=0, has_side_effects=True, vmem_limit_bytes=67_000_000
        ),
    )(
        tokens, first_gain.reshape(1, -1), mixer_gain.reshape(1, -1), head_gain.reshape(1, -1),
        log_decay, *sources,
    )


def shards_gathered(
    tokens, first_gain, mixer_gain, gate_weight, up_weight, down_weight,
    query_weight, key_weight, value_weight, head_gain, out_weight, log_decay,
):
    def rows_of(weight):
        return lax.all_gather(weight, "fs", axis=0, tiled=True)

    def columns_of(weight):
        return lax.all_gather(weight, "fs", axis=1, tiled=True)

    def times(left, right):
        return jnp.dot(left, right, preferred_element_type=jnp.float32)

    normed = norm_rows(tokens, first_gain)
    gathered = lax.all_gather(normed, "tp", axis=0, tiled=True)
    gate_sum = times(gathered, rows_of(gate_weight))
    hidden = (jax.nn.silu(gate_sum) * times(gathered, rows_of(up_weight))).astype(jnp.bfloat16)
    branch = times(hidden, columns_of(down_weight)).astype(jnp.bfloat16)
    summed = lax.psum_scatter(branch, "tp", scatter_dimension=0, tiled=True)
    after_first = (
        tokens.astype(jnp.float32) + 0.5 * summed.astype(jnp.float32)
    ).astype(jnp.bfloat16)
    gathered = lax.all_gather(norm_rows(after_first, mixer_gain), "tp", axis=0, tiled=True)
    queries, key_rows, value_rows = (
        times(gathered, rows_of(w)).astype(jnp.bfloat16)
        for w in (query_weight, key_weight, value_weight)
    )
    flat = retain(queries, key_rows, value_rows, head_gain, log_decay)
    branch = times(flat, columns_of(out_weight)).astype(jnp.bfloat16)
    summed = lax.psum_scatter(branch, "tp", scatter_dimension=0, tiled=True)
    return (after_first.astype(jnp.float32) + summed.astype(jnp.float32)).astype(jnp.bfloat16)


def shards(sizes, *args):
    depth = args[3].shape[0] * sizes["fs"]
    if sizes["grp"] == 2 and sizes["tp"] == 4 and sizes["fs"] == 4 and depth % (2 * sizes["fs"] * LANES) == 0:
        return shards_fused(sizes["fs"], *args)
    return shards_gathered(*args)


def solution(mesh):
    placed = (
        P(("grp", "fs", "tp"), None),
        P(),
        P(),
        P("fs", "tp"),
        P("fs", "tp"),
        P("tp", "fs"),
        P("fs", "tp"),
        P("fs", "tp"),
        P("fs", "tp"),
        P("tp"),
        P("tp", "fs"),
        P(None, "tp"),
    )
    return jax.shard_map(
        functools.partial(shards, dict(mesh.shape)),
        mesh=mesh, in_specs=placed, out_specs=P(("grp", "fs", "tp"), None), check_vma=False,
    )
```
